32 devices in a mesh: kv: 16 (over z, y, x), tp: 2 (over core).
Axes of the slice: x: 2, y: 2, z: 4, core: 2. Of those that a mesh axis runs over, the one named last changes fastest.
Arguments:
- hidden_in: bfloat16 [256, 2048], P('kv', 'tp'), may hold values from -6 to 6
- first_gain: bfloat16 [2048], P('tp'), may hold values from 0.099609375 to 1.8984375
- first_gate_proj: bfloat16 [2048, 5632], P('tp', 'kv'), may hold values from -0.125 to 0.125
- first_up_proj: bfloat16 [2048, 5632], P('tp', 'kv'), may hold values from -0.125 to 0.125
- first_down_proj: bfloat16 [5632, 2048], P('kv', 'tp'), may hold values from -0.078125 to 0.078125
- mix_gain: bfloat16 [2048], replicated, may hold values from 0.099609375 to 1.8984375
- query_weight: bfloat16 [2048, 1024], P(None, 'tp'), may hold values from -0.125 to 0.125
- forget_weight: bfloat16 [2048, 1024], P(None, 'tp'), may hold values from -0.125 to 0.125
- input_weight: bfloat16 [2048, 1024], P(None, 'tp'), may hold values from -0.125 to 0.125
- outgate_weight: bfloat16 [2048, 1024], P(None, 'tp'), may hold values from -0.125 to 0.125
- forget_floor: float32 [1024], P('tp'), may hold values from 0.05 to 0.95
- state_in: float32 [256, 8, 128, 128], P('kv', 'tp'), may hold values from -6 to 6
- out_gain: bfloat16 [1024], P('tp'), may hold values from 0.099609375 to 1.8984375
- mix_out_weight: bfloat16 [1024, 2048], P('tp'), may hold values from -0.1875 to 0.1875
- second_gain: bfloat16 [2048], P('tp'), may hold values from 0.099609375 to 1.8984375
- second_gate_proj: bfloat16 [2048, 5632], P('tp', 'kv'), may hold values from -0.125 to 0.125
- second_up_proj: bfloat16 [2048, 5632], P('tp', 'kv'), may hold values from -0.125 to 0.125
- second_down_proj: bfloat16 [5632, 2048], P('kv', 'tp'), may hold values from -0.078125 to 0.078125
Outputs:
- hidden_out: bfloat16 [256, 2048], P('kv', 'tp')
- state_out: float32 [256, 8, 128, 128], P('kv', 'tp')
The draws below stay inside these ranges and needn't reach their ends.
All inputs are finite; a program needn't handle non-finite values.
Results may differ from the reference program's by a relative error of at most 0.019.
Values may be sent and summed in bfloat16 or wider, within the bound.
No kernel may reach another device: no remote copies, remote signals or barrier semaphores. Data moves between devices by JAX's collectives and lax.ppermute only.
A program may use at most 64 MiB of HBM per device.

```python
import jax
import jax.numpy as jnp
from jax import lax

D = 2048
FF = 5632
HEADS = 8
HEAD = 128
BATCH = 256
HK = 1024
N_TP = 2


def levels(stream_key, shape, pieces, low, high):
    def one(position, parts):
        draws = jax.random.uniform(jax.random.fold_in(jax.random.fold_in(stream_key, 6), position), (parts,), jnp.float32, low / len(pieces), high / len(pieces))
        return jnp.repeat(jnp.exp(draws), shape[position] // parts).reshape((-1,) + (1,) * (len(shape) - position - 1))

    loudness = one(*pieces[0])
    for cut in pieces[1:]:
        loudness = loudness * one(*cut)
    return loudness


def gaussian(key, shape, scale, most, pieces=(), dtype=jnp.bfloat16):
    level = levels(key, shape, pieces, -0.22, 0.18) if pieces else 1.0
    result = jax.random.normal(key, shape, jnp.float32) * scale * level
    return jnp.minimum(jnp.maximum(result, -most), most).astype(dtype)


def setup_inputs(seed: int = 0) -> dict:
    arg_keys = jax.random.split(jax.random.key(seed), 19)
    return {
        "hidden_in": gaussian(arg_keys[0], (BATCH, D), 1.0, 6.0, ((0, 16), (1, 2))),
        "first_gain": jnp.clip(1.0 + 0.18 * jax.random.normal(arg_keys[1], (D,), jnp.float32), 0.099609375, 1.8984375).astype(jnp.bfloat16),
        "first_gate_proj": gaussian(arg_keys[2], (D, FF), D ** -0.5, 0.125, ((0, 2), (1, 16))),
        "first_up_proj": gaussian(arg_keys[3], (D, FF), D ** -0.5, 0.125, ((0, 2), (1, 16))),
        "first_down_proj": gaussian(arg_keys[4], (FF, D), FF ** -0.5, 0.078125, ((0, 16), (1, 2))),
        "mix_gain": jnp.clip(1.0 + 0.18 * jax.random.normal(arg_keys[5], (D,), jnp.float32), 0.099609375, 1.8984375).astype(jnp.bfloat16),
        "query_weight": gaussian(arg_keys[6], (D, HK), D ** -0.5, 0.125, ((1, 2),)),
        "forget_weight": gaussian(arg_keys[7], (D, HK), D ** -0.5, 0.125, ((1, 2),)),
        "input_weight": gaussian(arg_keys[8], (D, HK), D ** -0.5, 0.125, ((1, 2),)),
        "outgate_weight": gaussian(arg_keys[9], (D, HK), D ** -0.5, 0.125, ((1, 2),)),
        "forget_floor": jnp.clip(0.05 + 0.9 * jax.random.uniform(arg_keys[10], (HK,), jnp.float32) ** levels(arg_keys[10], (HK,), ((0, 2),), -0.2, 0.2), 0.05, 0.95),
        "state_in": gaussian(arg_keys[11], (BATCH, HEADS, HEAD, HEAD), 1.0, 6.0, ((0, 16), (1, 2)), jnp.float32),
        "out_gain": jnp.clip(1.0 + 0.18 * jax.random.normal(arg_keys[12], (HK,), jnp.float32), 0.099609375, 1.8984375).astype(jnp.bfloat16),
        "mix_out_weight": gaussian(arg_keys[13], (HK, D), HK ** -0.5, 0.1875, ((0, 2),)),
        "second_gain": jnp.clip(1.0 + 0.18 * jax.random.normal(arg_keys[14], (D,), jnp.float32), 0.099609375, 1.8984375).astype(jnp.bfloat16),
        "second_gate_proj": gaussian(arg_keys[15], (D, FF), D ** -0.5, 0.125, ((0, 2), (1, 16))),
        "second_up_proj": gaussian(arg_keys[16], (D, FF), D ** -0.5, 0.125, ((0, 2), (1, 16))),
        "second_down_proj": gaussian(arg_keys[17], (FF, D), FF ** -0.5, 0.078125, ((0, 16), (1, 2))),
    }


def feed_forward(hidden, norm_gain, gate_proj, up_proj, down_proj):
    values = hidden.astype(jnp.float32)
    inverse = lax.rsqrt(lax.optimization_barrier(jnp.mean(values * values, axis=1, keepdims=True)) + 1e-06)
    scaled = (values * norm_gain.astype(jnp.float32)).astype(jnp.bfloat16)
    gate_sum = jnp.dot(scaled, gate_proj, preferred_element_type=jnp.float32) * inverse
    up_sum = jnp.dot(scaled, up_proj, preferred_element_type=jnp.float32) * inverse
    inner_units = (jax.nn.silu(gate_sum) * up_sum).astype(jnp.bfloat16)
    down_sum = jnp.dot(inner_units, down_proj, preferred_element_type=jnp.float32)
    return (values + 0.5 * down_sum).astype(jnp.bfloat16)

def reference(hidden_in, first_gain, first_gate_proj, first_up_proj, first_down_proj, mix_gain, query_weight, forget_weight, input_weight, outgate_weight, forget_floor, state_in, out_gain, mix_out_weight, second_gain, second_gate_proj, second_up_proj, second_down_proj):
    first_out = feed_forward(hidden_in, first_gain, first_gate_proj, first_up_proj, first_down_proj)
    values = first_out.astype(jnp.float32)
    inverse = lax.rsqrt(lax.optimization_barrier(jnp.mean(values * values, axis=1, keepdims=True)) + 1e-06)
    normed = (values * inverse * mix_gain.astype(jnp.float32)).astype(jnp.bfloat16)
    batch_size = hidden_in.shape[0]

    def project(weight):
        return jnp.dot(normed, weight, preferred_element_type=jnp.float32).reshape(batch_size, HEADS, HEAD)
    query_vals = jax.nn.silu(project(query_weight))
    forget_pre = project(forget_weight)
    input_vals = project(input_weight)
    out_gate = project(outgate_weight)
    floor_vals = forget_floor.reshape(HEADS, HEAD)
    log_forget = jnp.logaddexp(jnp.log(floor_vals), jnp.log1p(-floor_vals) + jax.nn.log_sigmoid(forget_pre))
    key_vals = -jnp.expm1(log_forget)
    new_state = jnp.exp(log_forget)[..., None] * state_in + key_vals[..., None] * input_vals[:, :, None, :]
    readout = jnp.einsum('bhk,bhkv->bhv', query_vals, new_state, precision=lax.Precision.HIGHEST)
    normed_out = readout * lax.rsqrt(lax.optimization_barrier(jnp.mean(readout * readout, axis=-1, keepdims=True)) + 1e-05) * out_gain.astype(jnp.float32).reshape(HEADS, HEAD)
    gated_out = (normed_out * jax.nn.silu(out_gate)).reshape(batch_size, HK).astype(jnp.bfloat16)
    group_width = HK // N_TP
    gated_groups = gated_out.reshape(batch_size, N_TP, group_width).astype(jnp.float32)
    weight_groups = mix_out_weight.reshape(N_TP, group_width, D).astype(jnp.float32)
    partial_value = jnp.einsum('bgk,gkd->bgd', gated_groups, weight_groups).astype(jnp.bfloat16)
    mixed_sum = lax.optimization_barrier(jnp.sum(partial_value.astype(jnp.float32), axis=1))
    second_in = (values + mixed_sum).astype(jnp.bfloat16)
    hidden_out = feed_forward(second_in, second_gain, second_gate_proj, second_up_proj, second_down_proj)
    return (hidden_out, new_state)
```

```python
import jax
import jax.numpy as jnp
from jax import lax
from jax.sharding import PartitionSpec as P

BF = jnp.bfloat16
F32 = jnp.float32


def rounds_of(size):
    found = []
    stride = 1
    while stride < size:
        width = 4 if size % (stride * 4) == 0 else size // stride
        found.append((stride, width))
        stride *= width
    return found[::-1]


def swap(x, axis, size, mask):
    return lax.ppermute(x, axis, [(i, i ^ mask) for i in range(size)])


def gather_rows(x, axis, size):
    for stride, width in rounds_of(size):
        blocks = [x] + [swap(x, axis, size, j * stride) for j in range(1, width)]
        x = jnp.concatenate(blocks, axis=0)
    return x


def scatter_sum(x, axis, size):
    for stride, width in rounds_of(size)[::-1]:
        x = x.reshape(width, x.shape[0] // width, x.shape[1])
        sent = x.astype(BF)
        total = x[0].astype(F32)
        for j in range(1, width):
            total = total + swap(sent[j], axis, size, j * stride).astype(F32)
        x = total
    return x


def shards_for(n_kv, n_tp):
    def to_rows(x):
        core = lax.axis_index("tp")
        groups = x.reshape(n_tp, x.shape[0] // n_tp, x.shape[1])
        blocks = [lax.dynamic_index_in_dim(groups, core, 0, keepdims=False)]
        for j in range(1, n_tp):
            out = lax.dynamic_index_in_dim(groups, core ^ j, 0, keepdims=False)
            blocks.append(swap(out, "tp", n_tp, j))
        return jnp.concatenate(blocks, axis=1)

    def from_rows(x):
        core = lax.axis_index("tp")
        wide = x.reshape(x.shape[0], n_tp, x.shape[1] // n_tp)
        blocks = [wide[:, 0]] + [swap(wide[:, j], "tp", n_tp, j) for j in range(1, n_tp)]
        stacked = jnp.stack(blocks)
        if n_tp == 2:
            ordered = jnp.where(core == 0, stacked, stacked[::-1])
        else:
            ordered = stacked[jnp.arange(n_tp) ^ core]
        return ordered.reshape(-1, x.shape[1] // n_tp)

    def natural(x):
        core = lax.axis_index("tp")
        wide = x.reshape(x.shape[0], n_tp, x.shape[1] // n_tp)
        if n_tp == 2:
            wide = jnp.where(core == 0, wide, wide[:, ::-1])
        else:
            wide = wide[:, jnp.arange(n_tp) ^ core]
        return wide.reshape(x.shape)

    def xored(x):
        return natural(x)

    def everyones(w):
        return [w] + [swap(w, "tp", n_tp, j) for j in range(1, n_tp)]

    def feed_forward(rows, gain, gates, ups, downs):
        inverse = lax.rsqrt(jnp.mean(rows * rows, axis=1, keepdims=True) + 1e-06)
        scaled = (rows * inverse * gain).astype(BF)
        every = gather_rows(scaled, "kv", n_kv)
        cut = every.shape[1] // n_tp
        gate = 0.0
        up = 0.0
        for j in range(n_tp):
            part = every[:, j * cut : (j + 1) * cut]
            gate = gate + jnp.dot(part, gates[j], preferred_element_type=F32)
            up = up + jnp.dot(part, ups[j], preferred_element_type=F32)
        inner = (jax.nn.silu(gate) * up).astype(BF)
        down = jnp.concatenate([jnp.dot(inner, w, preferred_element_type=F32) for w in downs], axis=1)
        return rows + 0.5 * scatter_sum(down, "kv", n_kv)

    def shards(
        hidden_in,
        first_gain,
        first_gate_proj,
        first_up_proj,
        first_down_proj,
        mix_gain,
        query_weight,
        forget_weight,
        input_weight,
        outgate_weight,
        forget_floor,
        state_in,
        out_gain,
        mix_out_weight,
        second_gain,
        second_gate_proj,
        second_up_proj,
        second_down_proj,
    ):
        core = lax.axis_index("tp")
        gates1, ups1, downs1 = everyones(first_gate_proj), everyones(first_up_proj), everyones(first_down_proj)
        gates2, ups2, downs2 = everyones(second_gate_proj), everyones(second_up_proj), everyones(second_down_proj)
        gain1 = jnp.concatenate(everyones(first_gain)).astype(F32)[None, :]
        gain2 = jnp.concatenate(everyones(second_gain)).astype(F32)[None, :]

        rows = to_rows(hidden_in).astype(F32)
        x1 = feed_forward(rows, gain1, gates1, ups1, downs1).astype(BF)
        x1f = x1.astype(F32)
        inverse = lax.rsqrt(jnp.mean(x1f * x1f, axis=1, keepdims=True) + 1e-06)
        normed_rows = (natural(x1f * inverse) * mix_gain.astype(F32)).astype(BF)
        groups = [normed_rows] + [swap(normed_rows, "tp", n_tp, j) for j in range(1, n_tp)]
        if n_tp == 2:
            normed = jnp.where(
                core == 0, jnp.concatenate(groups, axis=0), jnp.concatenate(groups[::-1], axis=0)
            )
        else:
            normed = jnp.stack(groups)[jnp.arange(n_tp) ^ core].reshape(-1, normed_rows.shape[1])

        batch_here, heads_here, head_size = state_in.shape[0], state_in.shape[1], state_in.shape[2]

        def project(weight):
            return jnp.dot(normed, weight, preferred_element_type=F32).reshape(
                batch_here, heads_here, head_size
            )

        query_vals = jax.nn.silu(project(query_weight))
        forget_pre = project(forget_weight)
        input_vals = project(input_weight)
        out_gate = project(outgate_weight)
        floor_vals = forget_floor.reshape(heads_here, head_size)
        kept = floor_vals + (1.0 - floor_vals) * jax.nn.sigmoid(forget_pre)
        key_vals = (1.0 - floor_vals) * jax.nn.sigmoid(-forget_pre)
        new_state = kept[..., None] * state_in + key_vals[..., None] * input_vals[:, :, None, :]
        readout = jnp.sum(query_vals[..., None] * new_state, axis=2)
        normed_out = (
            readout
            * lax.rsqrt(jnp.mean(readout * readout, axis=-1, keepdims=True) + 1e-05)
            * out_gain.astype(F32).reshape(heads_here, head_size)
        )
        gated = (normed_out * jax.nn.silu(out_gate)).reshape(batch_here, -1).astype(BF)
        partial_value = jnp.dot(gated, mix_out_weight, preferred_element_type=F32).astype(BF)
        partial_groups = partial_value.reshape(n_tp, -1, partial_value.shape[1])
        mixed = lax.dynamic_index_in_dim(partial_groups, core, 0, keepdims=False).astype(F32)
        for j in range(1, n_tp):
            out = lax.dynamic_index_in_dim(partial_groups, core ^ j, 0, keepdims=False)
            mixed = mixed + swap(out, "tp", n_tp, j).astype(F32)
        x2 = (x1f + xored(mixed)).astype(BF)
        out_rows = feed_forward(x2.astype(F32), gain2, gates2, ups2, downs2).astype(BF)
        return (from_rows(out_rows), new_state)

    return shards


def solution(mesh):
    placed = (
        P("kv", "tp"),
        P("tp"),
        P("tp", "kv"),
        P("tp", "kv"),
        P("kv", "tp"),
        P(),
        P(None, "tp"),
        P(None, "tp"),
        P(None, "tp"),
        P(None, "tp"),
        P("tp"),
        P("kv", "tp", None, None),
        P("tp"),
        P("tp", None),
        P("tp"),
        P("tp", "kv"),
        P("tp", "kv"),
        P("kv", "tp"),
    )
    return jax.shard_map(
        shards_for(mesh.shape["kv"], mesh.shape["tp"]),
        mesh=mesh,
        in_specs=placed,
        out_specs=(P("kv", "tp"), P("kv", "tp", None, None)),
        check_vma=False,
    )
```

```python
import jax
import jax.numpy as jnp
from jax import lax
from jax.experimental import pallas as pl
from jax.experimental.pallas import tpu as pltpu
from jax.sharding import PartitionSpec as P

BF = jnp.bfloat16
F32 = jnp.float32


def rounds_of(size):
    found = []
    stride = 1
    while stride < size:
        width = 4 if size % (stride * 4) == 0 else size // stride
        found.append((stride, width))
        stride *= width
    return found[::-1]


def swap(x, axis, size, mask):
    return lax.ppermute(x, axis, [(i, i ^ mask) for i in range(size)])


def gather_rows(x, axis, size):
    blocks = [x]
    for stride, width in rounds_of(size):
        x = jnp.concatenate(blocks, axis=0)
        blocks = [x] + [swap(x, axis, size, j * stride) for j in range(1, width)]
    return blocks


def scatter_sum(own, sent, axis, size):
    for n, (stride, width) in enumerate(rounds_of(size)[::-1]):
        if n:
            parts = own.reshape(width, own.shape[0] // width, own.shape[1])
            own, sent = parts[0], [parts[j].astype(BF) for j in range(1, width)]
        for j in range(1, width):
            got = swap(sent[j - 1], axis, size, j * stride)
            own = own + got.astype(F32)
    return own


def expand(blocks, gates, ups, downs):
    count, cores = len(blocks), len(gates)
    height, model = blocks[0].shape
    cut = model // cores

    def body(*refs):
        block_refs = refs[:count]
        gate_refs, up_refs, down_refs = (
            refs[count + n * cores : count + (n + 1) * cores] for n in range(3)
        )
        out_refs = refs[count + 3 * cores :]
        values = jnp.concatenate([ref[...] for ref in block_refs], axis=0)

        def product(weight_refs):
            total = 0.0
            for j, ref in enumerate(weight_refs):
                total = total + lax.dot_general(
                    ref[...],
                    values[:, j * cut : (j + 1) * cut],
                    (((1,), (1,)), ((), ())),
                    preferred_element_type=F32,
                )
            return total

        gate = product(gate_refs)
        up = product(up_refs)
        inner = (gate * jax.nn.sigmoid(gate) * up).T.astype(BF)
        for j, ref in enumerate(down_refs):
            down = jnp.dot(inner, ref[...], preferred_element_type=F32)
            for n, out in enumerate(out_refs):
                out[:, j * cut : (j + 1) * cut] = down[n * height : (n + 1) * height].astype(out.dtype)

    vmem = pl.BlockSpec(memory_space=pltpu.VMEM)
    outs = [jax.ShapeDtypeStruct((height, model), F32 if n == 0 else BF) for n in range(count)]
    return pl.pallas_call(
        body,
        in_specs=[vmem] * (count + 3 * cores),
        out_specs=[vmem] * count,
        out_shape=outs,
        compiler_params=pltpu.CompilerParams(vmem_limit_bytes=8 * 1024 * 1024),
        name="expand",
    )(*blocks, *gates, *ups, *downs)


def load_to_vmem(arrays):
    count = len(arrays)

    def body(*refs):
        sems = refs[-1]
        copies = [
            pltpu.make_async_copy(refs[n], refs[count + n], sems.at[n]) for n in range(count)
        ]
        for copy in copies:
            copy.start()
        for copy in copies:
            copy.wait()

    size = sum(a.size * a.dtype.itemsize for a in arrays)
    return pl.pallas_call(
        body,
        in_specs=[pl.BlockSpec(memory_space=pltpu.HBM)] * count,
        out_specs=[pl.BlockSpec(memory_space=pltpu.VMEM)] * count,
        out_shape=[pltpu.VMEM(a.shape, a.dtype) for a in arrays],
        scratch_shapes=[pltpu.SemaphoreType.DMA((count,))],
        compiler_params=pltpu.CompilerParams(vmem_limit_bytes=1024 * 1024),
        cost_estimate=pl.CostEstimate(flops=size, transcendentals=0, bytes_accessed=size),
    )(*[pltpu.with_memory_space_constraint(a, pltpu.HBM) for a in arrays])


def mix_heads(rows, gain, query_w, forget_w, input_w, outgate_w, floor, out_gain, state, mix_out, axis):
    batch, heads, size, _ = state.shape
    wide = heads * size
    cores, group, model = rows.shape
    cut = model // cores

    def body(
        rows_ref, gain_ref, query_ref, forget_ref, input_ref, outgate_ref, floor_ref, out_gain_ref, state_ref, mix_ref,
        partial_ref, kept_ref, key_ref, ival_ref, read_buf,
    ):
        core = lax.axis_index(axis)
        ordered = []
        for g in range(cores):
            block = rows_ref[g ^ core].astype(F32)
            ordered.append(
                jnp.concatenate([block[:, (j ^ g) * cut : ((j ^ g) + 1) * cut] for j in range(cores)], axis=1)
            )
        values = jnp.concatenate(ordered, axis=0)
        scale = lax.rsqrt(jnp.mean(values * values, axis=1, keepdims=True) + 1e-06)
        normed = (values * scale * gain_ref[...].astype(F32)).astype(BF)

        def project(ref):
            return jnp.dot(normed, ref[...], preferred_element_type=F32)

        floors = floor_ref[...]
        forget_pre = project(forget_ref)
        kept = floors + (1.0 - floors) * jax.nn.sigmoid(forget_pre)
        key = (1.0 - floors) * jax.nn.sigmoid(-forget_pre)
        for h in range(heads):
            kept_ref[h] = kept[:, h * size : (h + 1) * size].T
            key_ref[h] = key[:, h * size : (h + 1) * size].T
        query = project(query_ref)
        query = query * jax.nn.sigmoid(query)
        weighted = query * kept
        overlap = query * key
        columns = [weighted[:, h * size : (h + 1) * size].T for h in range(heads)]
        ival = project(input_ref)
        ival_ref[...] = ival
        for b in range(batch):
            for h in range(heads):
                column = jnp.broadcast_to(columns[h][:, b : b + 1], (size, size))
                read = jnp.sum(column * state_ref[b, h], axis=0, keepdims=True)
                read_buf[b : b + 1, h * size : (h + 1) * size] = read
        gate = project(outgate_ref)
        gate = gate * jax.nn.sigmoid(gate)
        parts = []
        for h in range(heads):
            span = slice(h * size, (h + 1) * size)
            read = read_buf[:, span] + jnp.sum(overlap[:, span], axis=1, keepdims=True) * ival[:, span]
            unit = lax.rsqrt(jnp.mean(read * read, axis=1, keepdims=True) + 1e-05)
            parts.append((read * unit * out_gain_ref[:, span].astype(F32) * gate[:, span]).astype(BF))
        gated = jnp.concatenate(parts, axis=1)
        partial = jnp.dot(gated, mix_ref[...], preferred_element_type=F32)
        for g in range(cores):
            block = partial[g * group : (g + 1) * group]
            partial_ref[g ^ core] = jnp.concatenate(
                [block[:, (j ^ g) * cut : ((j ^ g) + 1) * cut] for j in range(cores)], axis=1
            ).astype(BF)

    vmem = pl.BlockSpec(memory_space=pltpu.VMEM)
    column_shape = jax.ShapeDtypeStruct((heads, size, batch), F32)
    return pl.pallas_call(
        body,
        in_specs=[vmem] * 10,
        out_specs=[vmem] * 4,
        out_shape=[
            jax.ShapeDtypeStruct((cores, group, mix_out.shape[1]), BF),
            column_shape,
            column_shape,
            jax.ShapeDtypeStruct((batch, wide), F32),
        ],
        scratch_shapes=[pltpu.VMEM((batch, wide), F32)],
        compiler_params=pltpu.CompilerParams(vmem_limit_bytes=4 * 1024 * 1024),
        name="mix_heads",
    )(rows, gain, query_w, forget_w, input_w, outgate_w, floor, out_gain, state, mix_out)


def next_state(kept, key, ival, state):
    batch, heads, size, _ = state.shape

    def body(kept_ref, key_ref, ival_ref, state_ref, out_ref, out_buf, sems):
        stores = [pltpu.make_async_copy(out_buf.at[b], out_ref.at[b], sems.at[b]) for b in range(batch)]
        for b in range(batch):
            for h in range(heads):
                kept_col = jnp.broadcast_to(kept_ref[h][:, b : b + 1], (size, size))
                key_col = jnp.broadcast_to(key_ref[h][:, b : b + 1], (size, size))
                row = ival_ref[b : b + 1, h * size : (h + 1) * size]
                out_buf[b, h] = kept_col * state_ref[b, h] + key_col * row
            stores[b].start()
        for copy in stores:
            copy.wait()

    vmem = pl.BlockSpec(memory_space=pltpu.VMEM)
    return pl.pallas_call(
        body,
        in_specs=[vmem] * 4,
        out_specs=pl.BlockSpec(memory_space=pltpu.HBM),
        out_shape=jax.ShapeDtypeStruct(state.shape, F32),
        scratch_shapes=[pltpu.VMEM(state.shape, F32), pltpu.SemaphoreType.DMA((batch,))],
        compiler_params=pltpu.CompilerParams(vmem_limit_bytes=6 * 1024 * 1024),
        cost_estimate=pl.CostEstimate(
            flops=3 * state.size, transcendentals=0, bytes_accessed=8 * state.size
        ),
        name="next_state",
    )(kept, key, ival, state)


def shards_for(n_kv, n_tp):
    def to_rows(x):
        core = lax.axis_index("tp")
        groups = x.reshape(n_tp, x.shape[0] // n_tp, x.shape[1])
        blocks = [lax.dynamic_index_in_dim(groups, core, 0, keepdims=False)]
        for j in range(1, n_tp):
            out = lax.dynamic_index_in_dim(groups, core ^ j, 0, keepdims=False)
            blocks.append(swap(out, "tp", n_tp, j))
        return jnp.concatenate(blocks, axis=1)

    def from_rows(x):
        core = lax.axis_index("tp")
        wide = x.reshape(x.shape[0], n_tp, x.shape[1] // n_tp)
        blocks = [wide[:, 0]] + [swap(wide[:, j], "tp", n_tp, j) for j in range(1, n_tp)]
        if n_tp == 2:
            rows = x.shape[0]
            return lax.dynamic_slice_in_dim(jnp.concatenate(blocks + blocks[:1]), core * rows, n_tp * rows)
        return jnp.stack(blocks)[jnp.arange(n_tp) ^ core].reshape(-1, x.shape[1] // n_tp)

    def everyones(w, own):
        return [own] + [swap(w, "tp", n_tp, j) for j in range(1, n_tp)]

    def feed_forward(rows, gain, gates, ups, downs):
        inverse = lax.rsqrt(jnp.mean(rows * rows, axis=1, keepdims=True) + 1e-06)
        scaled = (rows * inverse * gain).astype(BF)
        blocks = gather_rows(scaled, "kv", n_kv)
        own, *sent = expand(blocks, gates, ups, downs)
        return rows + 0.5 * scatter_sum(own, sent, "kv", n_kv)

    def shards(
        hidden_in,
        first_gain,
        first_gate_proj,
        first_up_proj,
        first_down_proj,
        mix_gain,
        query_weight,
        forget_weight,
        input_weight,
        outgate_weight,
        forget_floor,
        state_in,
        out_gain,
        mix_out_weight,
        second_gain,
        second_gate_proj,
        second_up_proj,
        second_down_proj,
    ):
        gate1, up1, down1, gate2, up2, down2 = (
            first_gate_proj.T,
            first_up_proj.T,
            first_down_proj,
            second_gate_proj.T,
            second_up_proj.T,
            second_down_proj,
        )
        gate1_v, up1_v, down1_v, state_v, mix_out_v = load_to_vmem([gate1, up1, down1, state_in, mix_out_weight])
        query_v, forget_v, input_v, outgate_v, gate2_v, up2_v, down2_v = load_to_vmem(
            [query_weight, forget_weight, input_weight, outgate_weight, gate2, up2, down2]
        )
        gates1, ups1, downs1 = everyones(gate1, gate1_v), everyones(up1, up1_v), everyones(down1, down1_v)
        gates2, ups2, downs2 = everyones(gate2, gate2_v), everyones(up2, up2_v), everyones(down2, down2_v)
        gain1 = jnp.concatenate(everyones(first_gain, first_gain)).astype(F32)[None, :]
        gain2 = jnp.concatenate(everyones(second_gain, second_gain)).astype(F32)[None, :]

        rows = to_rows(hidden_in).astype(F32)
        x1 = feed_forward(rows, gain1, gates1, ups1, downs1).astype(BF)
        x1f = x1.astype(F32)
        groups = jnp.stack([x1] + [swap(x1, "tp", n_tp, j) for j in range(1, n_tp)])
        partial_value, kept, key, ival = mix_heads(
            groups,
            mix_gain[None, :],
            query_v,
            forget_v,
            input_v,
            outgate_v,
            forget_floor[None, :],
            out_gain[None, :],
            state_v,
            mix_out_v,
            "tp",
        )
        new_state = next_state(kept, key, ival, state_v)
        mixed = partial_value[0].astype(F32)
        for j in range(1, n_tp):
            mixed = mixed + swap(partial_value[j], "tp", n_tp, j).astype(F32)
        x2 = (x1f + mixed).astype(BF)
        out_rows = feed_forward(x2.astype(F32), gain2, gates2, ups2, downs2).astype(BF)
        return (from_rows(out_rows), new_state)

    return shards


def solution(mesh):
    placed = (
        P("kv", "tp"),
        P("tp"),
        P("tp", "kv"),
        P("tp", "kv"),
        P("kv", "tp"),
        P(),
        P(None, "tp"),
        P(None, "tp"),
        P(None, "tp"),
        P(None, "tp"),
        P("tp"),
        P("kv", "tp", None, None),
        P("tp"),
        P("tp", None),
        P("tp"),
        P("tp", "kv"),
        P("tp", "kv"),
        P("kv", "tp"),
    )
    return jax.shard_map(
        shards_for(mesh.shape["kv"], mesh.shape["tp"]),
        mesh=mesh,
        in_specs=placed,
        out_specs=(P("kv", "tp"), P("kv", "tp", None, None)),
        check_vma=False,
    )
```
